32 devices in a mesh: grp: 2 (over y), sp: 4 (over z), tp: 4 (over x, core).
Axes of the slice: x: 2, y: 2, z: 4, core: 2. Of those that a mesh axis runs over, the one named last changes fastest.
Arguments:
- tokens: bfloat16 [8192, 2048], P(('grp', 'sp', 'tp')), parts along dimension 0, may hold values from -6 to 6
- step: float32 [8192], P(('grp', 'sp')), parts along dimension 0, may hold values from 0.2 to 3.75
- in_gain: float32 [2048], replicated, may hold values from 0.1 to 1.9
- in_proj: bfloat16 [2048, 512], P(None, 'tp'), may hold values from -0.125 to 0.125
- decay_rate: float32 [32, 64], P('tp'), may hold values from 2.4414063e-05 to 0.04
- frequency: float32 [32, 64], P('tp'), may hold values from 0.2 to 3
- input_map: float32 [2, 32, 64, 16], P(None, 'tp'), may hold values from -1 to 1
- readout: float32 [2, 32, 16, 64], P(None, 'tp'), may hold values from -0.75 to 0.75
- out_gain: float32 [512], replicated, may hold values from 0.1 to 1.9
- out_proj: bfloat16 [512, 2048], replicated, may hold values from -0.25 to 0.25
Outputs:
- mixed: bfloat16 [8192, 2048], P(('grp', 'sp', 'tp')), parts along dimension 0
The draws below stay inside these ranges and needn't reach their ends.
There are 2 independent parts, one for each index of `grp`. The reference program is written for one: setup_inputs(seed, part) draws one part's arguments, and reference() takes and returns one part's arrays. A program takes and returns all parts, laid end to end along the dimension named above; an argument that names none is the same for every part. Nothing has to cross between parts.
All inputs are finite; a program needn't handle non-finite values.
Results may differ from the reference program's by a relative error of at most 0.01.
Values may be sent and summed in bfloat16 or wider, within the bound.
A program may use at most 64 MiB of HBM per device.

```python
import jax
import jax.numpy as jnp
from jax import lax

D = 2048
CHANNELS = 512
GROUP_CH = 16
STATE = 64
GROUPS = 32
SEQ_DEV = 1024
TOKENS = 4096


def draw_step(key, part):
    level_key, fine_key = jax.random.split(key)
    levels = jnp.exp(jax.random.uniform(level_key, (TOKENS // SEQ_DEV,), jnp.float32, jnp.log(0.4), jnp.log(2.5)))
    fine = jnp.clip(1.0 + 0.25 * jax.random.normal(fine_key, (TOKENS,), jnp.float32), 0.5, 1.5)
    return jnp.repeat(levels, SEQ_DEV, total_repeat_length=TOKENS) * fine


def draw_decay_rate(key, part):
    pick_key, slow_key, fast_key = jax.random.split(key, 3)
    share = 0.5
    slow_mask = jax.random.uniform(pick_key, (GROUPS, STATE), jnp.float32) < share
    slow = jnp.exp(jax.random.uniform(slow_key, (GROUPS, STATE), jnp.float32, jnp.log(0.1), 0.0)) / TOKENS
    fast = jnp.exp(jax.random.uniform(fast_key, (GROUPS, STATE), jnp.float32, jnp.log(0.01), jnp.log(0.04)))
    return jnp.where(slow_mask, slow, fast)


def block_scale(rng, shape, pieces, low, top_value):
    factor_of, own = 1.0, jax.random.fold_in(rng, 6)
    for dim, blocks in pieces:
        heights = jnp.exp(jax.random.uniform(jax.random.fold_in(own, dim), (blocks,), jnp.float32, low / len(pieces), top_value / len(pieces)))
        factor_of = factor_of * jnp.repeat(heights, shape[dim] // blocks).reshape([-1 if axis == dim else 1 for axis in range(len(shape))])
    return factor_of


def gaussian(rng, shape, deviation, limit, cuts=(), kind=jnp.bfloat16):
    drawn = jax.random.normal(rng, shape, jnp.float32) * deviation
    if len(cuts) > 0:
        drawn = block_scale(rng, shape, cuts, -0.22, 0.18) * drawn
    return jnp.clip(drawn, min=-limit, max=limit).astype(kind)


def setup_inputs(seed: int = 0, part: int = 0) -> dict:
    splits = jax.random.split(jax.random.key(seed), 11)
    part_splits = jax.random.split(jax.random.fold_in(splits[10], part), 11)
    return {
        "tokens": gaussian(part_splits[0], (TOKENS, D), 1.0, 6.0, ((0, 16),)),
        "step": draw_step(jax.random.fold_in(jax.random.fold_in(splits[10], part), 71), part),
        "in_gain": jnp.clip(1.0 + 0.18 * jax.random.normal(splits[2], (D,), jnp.float32), 0.1, 1.9),
        "in_proj": gaussian(splits[3], (D, CHANNELS), D ** -0.5, 0.125, ((1, 4),)),
        "decay_rate": draw_decay_rate(jax.random.fold_in(splits[10], 71), part),
        "frequency": jnp.clip(0.2 + 2.8 * jax.random.uniform(splits[5], (GROUPS, STATE), jnp.float32) ** block_scale(splits[5], (GROUPS, STATE), ((0, 4),), -0.2, 0.2), 0.2, 3.0),
        "input_map": gaussian(splits[6], (2, GROUPS, STATE, GROUP_CH), (2 * GROUP_CH) ** -0.5, 1.0, ((1, 4),), jnp.float32),
        "readout": gaussian(splits[7], (2, GROUPS, GROUP_CH, STATE), STATE ** -0.5, 0.75, ((1, 4),), jnp.float32),
        "out_gain": jnp.clip(1.0 + 0.18 * jax.random.normal(splits[8], (CHANNELS,), jnp.float32), 0.1, 1.9),
        "out_proj": gaussian(splits[9], (CHANNELS, D), CHANNELS ** -0.5, 0.25),
    }


HIGHEST = lax.Precision.HIGHEST

def compose(earlier, later):
    a_re, a_im, b_re, b_im = earlier
    c_re, c_im, d_re, d_im = later
    return (c_re * a_re - c_im * a_im, c_re * a_im + c_im * a_re, c_re * b_re - c_im * b_im + d_re, c_re * b_im + c_im * b_re + d_im)

def rms_rows(values, gain):
    values = values.astype(jnp.float32)
    scaled = values * lax.rsqrt(lax.optimization_barrier(jnp.mean(values * values, axis=-1, keepdims=True)) + 1e-06)
    return (scaled * gain).astype(jnp.bfloat16)

def transition(times, decay_rate, frequency):
    spans = times.astype(jnp.float32)[:, None, None]
    magnitude = jnp.exp(-decay_rate[None] * spans)
    a_re = magnitude * jnp.cos(frequency[None] * spans)
    a_im = magnitude * jnp.sin(frequency[None] * spans)
    lam_re = -decay_rate
    denom = lam_re * lam_re + frequency * frequency
    n_re = a_re - 1.0
    z_re = (n_re * lam_re + a_im * frequency) / denom
    z_im = (a_im * lam_re - n_re * frequency) / denom
    return (a_re, a_im, z_re, z_im)

def injection(drive, input_map, z_re, z_im):
    groups = input_map.shape[1]
    grouped = drive.astype(jnp.float32).reshape(drive.shape[0], groups, -1)
    push_re = jnp.einsum('tgh,gph->tgp', grouped, input_map[0], precision=HIGHEST)
    push_im = jnp.einsum('tgh,gph->tgp', grouped, input_map[1], precision=HIGHEST)
    return (z_re * push_re - z_im * push_im, z_re * push_im + z_im * push_re)

def response(s_re, s_im, readout):
    value = jnp.einsum('tgp,ghp->tgh', s_re, readout[0], precision=HIGHEST) - jnp.einsum('tgp,ghp->tgh', s_im, readout[1], precision=HIGHEST)
    value = value.reshape(s_re.shape[0], -1)
    return jax.nn.gelu(value, approximate=True).astype(jnp.bfloat16)

def reference(tokens, step, in_gain, in_proj, decay_rate, frequency, input_map, readout, out_gain, out_proj):
    normed = rms_rows(tokens, in_gain)
    drive = jnp.dot(normed, in_proj, preferred_element_type=jnp.float32).astype(jnp.bfloat16)
    block_count = TOKENS // SEQ_DEV
    drive_blocks = drive.reshape(block_count, SEQ_DEV, -1)
    time_blocks = step.reshape(block_count, SEQ_DEV)
    zero = jnp.zeros(decay_rate.shape, jnp.float32)

    def advance(carry, piece):
        drive_part, time_part = piece
        a_re, a_im, z_re, z_im = transition(time_part, decay_rate, frequency)
        i_re, i_im = injection(drive_part, input_map, z_re, z_im)
        c_re, c_im, s_re, s_im = lax.associative_scan(compose, (a_re, a_im, i_re, i_im), axis=0)
        s_re = s_re + c_re * carry[0] - c_im * carry[1]
        s_im = s_im + c_re * carry[1] + c_im * carry[0]
        return ((s_re[-1], s_im[-1]), response(s_re, s_im, readout))
    _, answer = lax.scan(advance, (zero, zero), (drive_blocks, time_blocks))
    answer = answer.reshape(TOKENS, -1)
    shaped = rms_rows(answer, out_gain)
    return jnp.dot(shaped, out_proj, preferred_element_type=jnp.float32).astype(jnp.bfloat16)
```

```python
import functools
import math

import jax
import jax.numpy as jnp
from jax import lax
from jax.experimental import pallas as pl
from jax.experimental.pallas import tpu as pltpu
from jax.sharding import PartitionSpec as P

F32 = jnp.float32
BF16 = jnp.bfloat16
MESH = pl.DeviceIdType.MESH
CHUNKS = 4
STRIP = 16
COLS = 512
COS = (0.9999992107823232, -19.738980355764078, 64.9286574210355, -85.2716215343227, 58.79049212023138, -21.071105627794083)
SIN = (6.28318491649543, -41.34158923268886, 81.59994332979169, -76.61447253134615, 41.34288235500672, -12.471243535733244)
FORM = dict(preferred_element_type=F32)


def poly(coefs, z):
    total = coefs[-1] * z + coefs[-2]
    for value in coefs[-3::-1]:
        total = total * z + value
    return total


def turn(phase):
    r = phase - jnp.round(phase)
    z = r * r
    return poly(COS, z), poly(SIN, z) * r


def kernel(
    n, n_tp, tok_hbm, step_ref, gain_ref, proj_hbm, rf_ref, bc_ref, ogain_ref, oproj_hbm, out_ref,
    tok, normed, w_in, oproj, p_re, p_im, d_re, d_im, p_cat, y_loc,
    wide, acc, state, times, rf_all, bc_all, rf8, e_send, e_recv, dt_send, dt_recv,
    c_w, s_w, x_ref, tab, shaped,
    load_sem, small_sem, small_send, w_recv, w_send, bc_recv, bc_send,
    e_rsem, e_ssem, dt_rsem, dt_ssem,
):
    grp, sp, tp = lax.axis_index("grp"), lax.axis_index("sp"), lax.axis_index("tp")
    rank = sp * n_tp + tp
    rows = tok.shape[0]
    depth = w_in.shape[1]
    half = depth // 2
    piece = half // CHUNKS
    lanes = rf_all.shape[-1]
    blocks = lanes // 128

    def place(r):
        return {"sp": r // n_tp, "tp": lax.rem(r, n_tp)}

    peer = [None] + [{"tp": tp ^ m} for m in range(1, n_tp)]
    across = {"grp": 1 - grp}

    loads = [
        pltpu.make_async_copy(proj_hbm, w_in.at[0], load_sem.at[0]),
        pltpu.make_async_copy(tok_hbm, tok, load_sem.at[1]),
        pltpu.make_async_copy(oproj_hbm, oproj, load_sem.at[2]),
    ]
    for copy in loads:
        copy.start()

    barrier = pltpu.get_barrier_semaphore()

    def greet(k, _):
        pl.semaphore_signal(barrier, inc=1, device_id=place(lax.rem(rank + k, n)), device_id_type=MESH)
        return 0

    lax.fori_loop(1, n, greet, 0)
    pl.semaphore_signal(barrier, inc=1, device_id=across, device_id_type=MESH)

    step_row = step_ref[...]
    row_id = lax.broadcasted_iota(jnp.int32, (rows, rows), 0)
    col_id = lax.broadcasted_iota(jnp.int32, (rows, rows), 1)
    causal = col_id <= row_id
    elapsed = jnp.sum(jnp.where(causal, jnp.broadcast_to(step_row, (rows, rows)), 0.0), axis=1, keepdims=True)
    times[...] = jnp.broadcast_to(elapsed, (rows, 128))
    dt_send[...] = jnp.broadcast_to(jnp.sum(step_row, axis=1, keepdims=True), (1, 128))
    lower = causal.astype(F32).astype(BF16)

    loads[0].wait()
    pl.semaphore_wait(barrier, n)

    started = []

    def send(src, dst, ssem, rsem, where):
        copy = pltpu.make_async_remote_copy(
            src_ref=src, dst_ref=dst, send_sem=ssem, recv_sem=rsem, device_id=where, device_id_type=MESH
        )
        copy.start()
        started.append(copy)
        return copy

    def arrived(dst, rsem):
        pltpu.make_async_copy(dst, dst, rsem).wait()

    for m in range(1, n_tp):
        send(rf_ref, rf_all.at[m], small_send.at[m], small_sem.at[m], peer[m])
    own_half = grp * half
    other_half = (1 - grp) * half
    for c in range(CHUNKS):
        part = pl.ds(pl.multiple_of(own_half + c * piece, 128), piece)
        send(w_in.at[0, part], w_in.at[2, part], w_send.at[0, c], w_recv.at[0, c], peer[2])
    send(w_in.at[0], w_in.at[1], w_send.at[1, 0], w_recv.at[1, 0], peer[1])
    send(bc_ref.at[grp], bc_all.at[2, grp], bc_send.at[0], bc_recv.at[0], peer[2])
    send(bc_ref, bc_all.at[1], bc_send.at[1], bc_recv.at[1], peer[1])

    def send_times(r, _):
        copy = pltpu.make_async_remote_copy(
            src_ref=dt_send, dst_ref=dt_recv.at[rank], send_sem=dt_ssem.at[r], recv_sem=dt_rsem.at[rank],
            device_id=place(r), device_id_type=MESH,
        )
        copy.start()
        return 0

    lax.fori_loop(rank + 1, n, send_times, 0)

    rf_all[0] = rf_ref[...]
    bc_all[0] = bc_ref[...]

    loads[1].wait()
    gain = gain_ref[...]

    def norm_strip(i, _):
        at = pl.ds(pl.multiple_of(i * STRIP, STRIP), STRIP)
        value = tok[at, :].astype(F32)
        scale = lax.rsqrt(jnp.mean(value * value, axis=1, keepdims=True) + 1e-6)
        normed[at, :] = (value * scale * gain).astype(BF16)
        return 0

    lax.fori_loop(0, rows // STRIP, norm_strip, 0)

    def forward(c, mine):
        base = own_half if mine else other_half
        part = pl.ds(pl.multiple_of(base + c * piece, 128), piece)
        way = 0 if mine else 2
        arrived(w_in.at[2, part], w_recv.at[way, c])
        if mine:
            send(w_in.at[2, part], w_in.at[2, part], w_send.at[2, c], w_recv.at[2, c], across)
        send(w_in.at[2, part], w_in.at[3, part], w_send.at[3 if mine else 4, c], w_recv.at[3 if mine else 4, c], peer[1])

    def tables(m):
        rate = rf_all[m, 0:1, :]
        freq = rf_all[m, 1:2, :]
        first = lax.broadcasted_iota(jnp.int32, (STRIP, lanes), 0) == 0

        def strip(i, before):
            br, bi = before
            at = pl.ds(pl.multiple_of(i * STRIP, STRIP), STRIP)
            t = times[at, 0:1]
            c, s = turn(t * freq)
            load = t * rate
            small = jnp.exp(-load)
            large = jnp.exp(load)
            pr, pi = small * c, small * s
            p_re[m, at, :] = pr
            p_im[m, at, :] = pi
            p_cat[m, at, 0:lanes] = pr.astype(BF16)
            p_cat[m, at, lanes:] = pi.astype(BF16)
            qr, qi = large * c, -large * s
            d_re[m, at, :] = jnp.where(first, pltpu.roll(br, 1, 0), pltpu.roll(qr, 1, 0)) - qr
            d_im[m, at, :] = jnp.where(first, pltpu.roll(bi, 1, 0), pltpu.roll(qi, 1, 0)) - qi
            return qr, qi

        lax.fori_loop(0, rows // STRIP, strip, (jnp.ones((STRIP, lanes), F32), jnp.zeros((STRIP, lanes), F32)))

    per = 16
    mask_r = lax.broadcasted_iota(jnp.int32, (128, lanes), 0) // per
    mask_c = lax.broadcasted_iota(jnp.int32, (128, lanes), 1) // (lanes // (128 // per))
    same = mask_r == mask_c

    def spread(compact):
        return jnp.where(same, jnp.concatenate([compact.astype(F32)] * (128 // per), axis=0), 0.0)

    def local(m):
        tab[:, 0:lanes] = spread(bc_all[m, 0, 0]).astype(BF16)
        tab[:, lanes:] = spread(bc_all[m, 0, 1]).astype(BF16)
        drive = jnp.dot(normed[...], w_in[m], **FORM).astype(BF16)
        acc[...] = jnp.dot(drive, tab[...], **FORM)

        def weigh(i, _):
            at = pl.ds(pl.multiple_of(i * STRIP, STRIP), STRIP)
            vr, vi = acc[at, 0:lanes], acc[at, lanes:]
            dr, di = d_re[m, at, :], d_im[m, at, :]
            wide[at, 0:lanes] = (dr * vr - di * vi).astype(BF16)
            wide[at, lanes:] = (dr * vi + di * vr).astype(BF16)
            return 0

        lax.fori_loop(0, rows // STRIP, weigh, 0)
        acc[...] = jnp.dot(lower, wide[...], **FORM)
        last = pl.ds(rows - 1, 1)
        for b in range(blocks):
            at = pl.ds(b * 128, 128)
            ar, ai = acc[last, at], acc[last, pl.ds(lanes + b * 128, 128)]
            pr, pi = p_re[m, last, at], p_im[m, last, at]
            e_send[m, pl.ds(b, 1), :] = pr * ar - pi * ai
            e_send[m, pl.ds(blocks + b, 1), :] = pr * ai + pi * ar
        owner = tp ^ m

        def send_end(r, _):
            copy = pltpu.make_async_remote_copy(
                src_ref=e_send.at[m], dst_ref=e_recv.at[rank, owner], send_sem=e_ssem.at[r, m],
                recv_sem=e_rsem.at[rank, owner], device_id=place(r), device_id_type=MESH,
            )
            copy.start()
            return 0

        lax.fori_loop(rank + 1, n, send_end, 0)

        def rotate(i, _):
            at = pl.ds(pl.multiple_of(i * STRIP, STRIP), STRIP)
            ar, ai = acc[at, 0:lanes], acc[at, lanes:]
            pr, pi = p_re[m, at, :], p_im[m, at, :]
            state[at, 0:lanes] = (pr * ar - pi * ai).astype(BF16)
            state[at, lanes:] = (pr * ai + pi * ar).astype(BF16)
            return 0

        lax.fori_loop(0, rows // STRIP, rotate, 0)
        tab[:, 0:lanes] = spread(bc_all[m, 1, 0]).astype(BF16)
        tab[:, lanes:] = (-spread(bc_all[m, 1, 1])).astype(BF16)
        y_loc[m] = lax.dot_general(state[...], tab[...], (((1,), (1,)), ((), ())), **FORM)

    tables(0)
    local(0)
    for m in range(1, n_tp):
        arrived(rf_all.at[m], small_sem.at[m])
    tables(1)
    for c in range(CHUNKS):
        forward(c, True)
    arrived(bc_all.at[2, grp], bc_recv.at[0])
    send(bc_all.at[2, grp], bc_all.at[2, grp], bc_send.at[2], bc_recv.at[2], across)
    send(bc_all.at[2, grp], bc_all.at[3, grp], bc_send.at[3], bc_recv.at[3], peer[1])
    tables(2)
    for c in range(CHUNKS):
        forward(c, False)
    arrived(bc_all.at[2, 1 - grp], bc_recv.at[2])
    send(bc_all.at[2, 1 - grp], bc_all.at[3, 1 - grp], bc_send.at[4], bc_recv.at[4], peer[1])
    arrived(w_in.at[1], w_recv.at[1, 0])
    arrived(bc_all.at[1], bc_recv.at[1])
    local(1)
    tables(3)
    local(2)
    sign = jnp.where(lax.broadcasted_iota(jnp.int32, (2 * blocks, 128), 0) < blocks, -1.0, 1.0)
    for m in range(n_tp):
        for b in range(blocks):
            at = pl.ds(b * 128, 128)
            for kind in range(2):
                value = rf_all[m, kind:kind + 1, at]
                rf8[m, kind, pl.ds(b, 1), :] = value
                rf8[m, kind, pl.ds(blocks + b, 1), :] = value

    def weight(k, since):
        j = rank - 1 - k
        arrived(dt_recv.at[j], dt_rsem.at[j])
        for m in range(n_tp):
            c, s = turn(since * rf8[m, 1])
            shrink = jnp.exp(-since * rf8[m, 0])
            c_w[j, m] = shrink * c
            s_w[j, m] = shrink * s * sign
        return since + dt_recv[j]

    lax.fori_loop(0, rank, weight, jnp.zeros((1, 128), F32))

    for c in range(CHUNKS):
        arrived(w_in.at[3, pl.ds(pl.multiple_of(own_half + c * piece, 128), piece)], w_recv.at[3, c])
        arrived(w_in.at[3, pl.ds(pl.multiple_of(other_half + c * piece, 128), piece)], w_recv.at[4, c])
    arrived(bc_all.at[3, grp], bc_recv.at[3])
    arrived(bc_all.at[3, 1 - grp], bc_recv.at[4])
    local(3)

    total = jnp.zeros((rows, 1), F32)
    for m in range(n_tp):
        owner = tp ^ m

        def take(j, x):
            arrived(e_recv.at[j, owner], e_rsem.at[j, owner])
            value = e_recv[j, owner]
            return x + c_w[j, m] * value + s_w[j, m] * pltpu.roll(value, blocks, 0)

        x_ref[...] = lax.fori_loop(0, rank, take, jnp.zeros((2 * blocks, 128), F32))
        cr = spread(bc_all[m, 1, 0])
        ci = spread(bc_all[m, 1, 1])
        for b in range(blocks):
            at = slice(b * 128, (b + 1) * 128)
            xr, xi = x_ref[pl.ds(b, 1), :], x_ref[pl.ds(blocks + b, 1), :]
            tab[:, b * 128:(b + 1) * 128] = (cr[:, at] * xr - ci[:, at] * xi).astype(BF16)
            tab[:, lanes + b * 128:lanes + (b + 1) * 128] = (-(cr[:, at] * xi + ci[:, at] * xr)).astype(BF16)
        v = y_loc[m] + lax.dot_general(p_cat[m], tab[...], (((1,), (1,)), ((), ())), **FORM)
        v = 0.5 * v * (1.0 + jnp.tanh(0.7978845608 * (v + 0.044715 * (v * v * v))))
        v = v.astype(BF16).astype(F32)
        y_loc[m] = v
        total = total + jnp.sum(v * v, axis=1, keepdims=True)
    scale = lax.rsqrt(total * (1.0 / (n_tp * 128)) + 1e-6)
    for m in range(n_tp):
        owner = tp ^ m
        shaped[:, pl.ds(pl.multiple_of(owner * 128, 128), 128)] = (y_loc[m] * scale * ogain_ref[owner]).astype(BF16)
    loads[2].wait()
    for c in range(out_ref.shape[1] // COLS):
        at = slice(c * COLS, (c + 1) * COLS)
        out_ref[:, at] = jnp.dot(shaped[...], oproj[:, at], **FORM).astype(BF16)

    for copy in started:
        copy.wait_send()

    def drain(r, _):
        pltpu.make_async_copy(dt_send, dt_send, dt_ssem.at[r]).wait()
        for m in range(n_tp):
            pltpu.make_async_copy(e_send.at[m], e_send.at[m], e_ssem.at[r, m]).wait()
        return 0

    lax.fori_loop(rank + 1, n, drain, 0)


def on_device(
    tokens, step, in_gain, in_proj, decay_rate, frequency, input_map, readout, out_gain, out_proj
):
    n_tp, n_sp = lax.axis_size("tp"), lax.axis_size("sp")
    n = n_tp * n_sp
    rows, width = tokens.shape
    groups, size = decay_rate.shape
    lanes = groups * size
    inner = input_map.shape[3]
    chans = groups * inner
    assert n_tp == 4 and chans == 128 and inner == 16 and lax.axis_size("grp") == 2
    own_step = lax.dynamic_slice(step, (lax.axis_index("tp") * rows,), (rows,)).reshape(1, rows)
    rate, freq = decay_rate.reshape(1, lanes), frequency.reshape(1, lanes)
    rf = jnp.concatenate([rate, freq * (0.5 / math.pi)], axis=0)
    maps = input_map.transpose(0, 3, 1, 2).reshape(2, inner, lanes)
    norm = 1.0 / (rate * rate + freq * freq)
    b_re = (freq * maps[1] - rate * maps[0]) * norm
    b_im = -(freq * maps[0] + rate * maps[1]) * norm
    reads = readout.transpose(0, 2, 1, 3).reshape(2, inner, lanes)
    bc = jnp.stack([jnp.stack([b_re, b_im]), reads]).astype(BF16)
    vmem, dma = pltpu.VMEM, pltpu.SemaphoreType.DMA
    full = pl.BlockSpec(memory_space=pltpu.VMEM)
    away = pl.BlockSpec(memory_space=pl.ANY)
    tile = (2 * lanes // 128, 128)
    return pl.pallas_call(
        functools.partial(kernel, n, n_tp),
        out_shape=jax.ShapeDtypeStruct((rows, width), BF16),
        in_specs=[away, full, full, away, full, full, full, away],
        out_specs=full,
        scratch_shapes=[
            vmem((rows, width), BF16), vmem((rows, width), BF16), vmem((n_tp, width, chans), BF16),
            vmem((n_tp * chans, width), BF16),
            vmem((n_tp, rows, lanes), F32), vmem((n_tp, rows, lanes), F32),
            vmem((n_tp, rows, lanes), F32), vmem((n_tp, rows, lanes), F32),
            vmem((n_tp, rows, 2 * lanes), BF16),
            vmem((n_tp, rows, chans), F32),
            vmem((rows, 2 * lanes), BF16), vmem((rows, 2 * lanes), F32), vmem((rows, 2 * lanes), BF16),
            vmem((rows, 128), F32), vmem((n_tp, 2, lanes), F32), vmem((n_tp, 2, 2, inner, lanes), BF16),
            vmem((n_tp, 2) + tile, F32),
            vmem((n_tp,) + tile, F32), vmem((n, n_tp) + tile, F32),
            vmem((1, 128), F32), vmem((n, 1, 128), F32),
            vmem((n, n_tp) + tile, F32), vmem((n, n_tp) + tile, F32), vmem(tile, F32),
            vmem((chans, 2 * lanes), BF16), vmem((rows, n_tp * chans), BF16),
            dma((3,)), dma((n_tp,)), dma((n_tp,)), dma((5, CHUNKS)), dma((5, CHUNKS)), dma((5,)), dma((5,)),
            dma((n, n_tp)), dma((n, n_tp)), dma((n,)), dma((n,)),
        ],
        compiler_params=pltpu.CompilerParams(collective_id=0, has_side_effects=True, vmem_limit_bytes=60 * 2**20),
    )(tokens, own_step, in_gain.reshape(1, width), in_proj, rf, bc, out_gain.reshape(n_tp, 1, chans), out_proj)


def solution(mesh):
    placed = (
        P(("grp", "sp", "tp"), None),
        P(("grp", "sp")),
        P(),
        P(None, "tp"),
        P("tp", None),
        P("tp", None),
        P(None, "tp", None, None),
        P(None, "tp", None, None),
        P(),
        P(),
    )
    return jax.shard_map(
        on_device,
        mesh=mesh,
        in_specs=placed,
        out_specs=P(("grp", "sp", "tp"), None),
        check_vma=False,
    )
```

```python
import functools
import math

import jax
import jax.numpy as jnp
from jax import lax
from jax.experimental import pallas as pl
from jax.experimental.pallas import tpu as pltpu
from jax.sharding import PartitionSpec as P

F32 = jnp.float32
BF16 = jnp.bfloat16
MESH = pl.DeviceIdType.MESH
CHUNKS = 4
STRIP = 16
COS = (0.9999992107823232, -19.738980355764078, 64.9286574210355, -85.2716215343227, 58.79049212023138, -21.071105627794083)
SIN = (6.28318491649543, -41.34158923268886, 81.59994332979169, -76.61447253134615, 41.34288235500672, -12.471243535733244)
WHOLE = 12582912.0
FORM = dict(preferred_element_type=F32)


def poly(coefs, z):
    total = coefs[-1] * z + coefs[-2]
    for value in coefs[-3::-1]:
        total = total * z + value
    return total


def turn(phase):
    r = phase - ((phase + WHOLE) - WHOLE)
    z = r * r
    return poly(COS, z), poly(SIN, z) * r


def kernel(
    n, n_tp, tok_hbm, step_ref, gain_ref, proj_hbm, rate_ref, freq_ref, map_ref, read_ref, ogain_ref, out_ref,
    tok, normed, w_in, p_re, p_im, d_re, d_im, p_cat, y_loc,
    wide, acc, state, times, rf_pack, rf_all, bc_all, rf8, e_send, e_recv, dt_send, dt_recv,
    c_w, s_w, x_ref, tab,
    load_sem, small_sem, small_send, w_recv, w_send, bc_recv, bc_send,
    e_rsem, e_ssem, dt_rsem, dt_ssem,
):
    grp, sp, tp = lax.axis_index("grp"), lax.axis_index("sp"), lax.axis_index("tp")
    rank = sp * n_tp + tp
    rows = tok.shape[0]
    depth = w_in.shape[1]
    half = depth // 2
    piece = half // CHUNKS
    lanes = rf_all.shape[-1]
    blocks = lanes // 128

    def place(r):
        return {"sp": r // n_tp, "tp": lax.rem(r, n_tp)}

    peer = [None] + [{"tp": tp ^ m} for m in range(1, n_tp)]
    across = {"grp": 1 - grp}

    loads = [
        pltpu.make_async_copy(proj_hbm, w_in.at[0], load_sem.at[0]),
        pltpu.make_async_copy(tok_hbm, tok, load_sem.at[1]),
    ]
    for copy in loads:
        copy.start()

    barrier = pltpu.get_barrier_semaphore()

    def greet(k, _):
        pl.semaphore_signal(barrier, inc=1, device_id=place(lax.rem(rank + k, n)), device_id_type=MESH)
        return 0

    lax.fori_loop(1, n, greet, 0)
    pl.semaphore_signal(barrier, inc=1, device_id=across, device_id_type=MESH)

    step_row = step_ref[:, pl.ds(pl.multiple_of(tp * rows, 128), rows)]
    row_id = lax.broadcasted_iota(jnp.int32, (rows, rows), 0)
    col_id = lax.broadcasted_iota(jnp.int32, (rows, rows), 1)
    causal = col_id <= row_id
    elapsed = jnp.sum(jnp.where(causal, jnp.broadcast_to(step_row, (rows, rows)), 0.0), axis=1, keepdims=True)
    times[...] = jnp.broadcast_to(elapsed, (rows, 128))
    dt_send[...] = jnp.broadcast_to(jnp.sum(step_row, axis=1, keepdims=True), (1, 128))
    lower = causal.astype(F32).astype(BF16)

    size = rate_ref.shape[1]
    per = map_ref.shape[1] // rate_ref.shape[0]
    rate, freq = rate_ref[...], freq_ref[...]
    rf_pack[0] = jnp.concatenate([rate, freq * (0.5 / math.pi)], axis=1)

    def rows_of(value):
        return jnp.concatenate([jnp.broadcast_to(value[g:g + 1], (per, size)) for g in range(value.shape[0])], axis=0)

    norm = 1.0 / (rate * rate + freq * freq)
    r_n, f_n = rows_of(-rate * norm), rows_of(freq * norm)
    bc_all[0, 0] = jnp.concatenate(
        [f_n * map_ref[1] + r_n * map_ref[0], r_n * map_ref[1] - f_n * map_ref[0]], axis=1
    ).astype(BF16)
    bc_all[0, 1] = jnp.concatenate([read_ref[0], read_ref[1]], axis=1).astype(BF16)

    loads[0].wait()
    pl.semaphore_wait(barrier, n)

    started = []

    def send(src, dst, ssem, rsem, where):
        copy = pltpu.make_async_remote_copy(
            src_ref=src, dst_ref=dst, send_sem=ssem, recv_sem=rsem, device_id=where, device_id_type=MESH
        )
        copy.start()
        started.append(copy)
        return copy

    def arrived(dst, rsem):
        pltpu.make_async_copy(dst, dst, rsem).wait()

    for m in range(1, n_tp):
        send(rf_pack.at[0], rf_pack.at[m], small_send.at[m], small_sem.at[m], peer[m])
    own_half = grp * half
    other_half = (1 - grp) * half
    for c in range(CHUNKS):
        part = pl.ds(pl.multiple_of(own_half + c * piece, 128), piece)
        send(w_in.at[0, part], w_in.at[2, part], w_send.at[0, c], w_recv.at[0, c], peer[2])
    send(w_in.at[0], w_in.at[1], w_send.at[1, 0], w_recv.at[1, 0], peer[1])
    send(bc_all.at[0, grp], bc_all.at[2, grp], bc_send.at[0], bc_recv.at[0], peer[2])
    send(bc_all.at[0], bc_all.at[1], bc_send.at[1], bc_recv.at[1], peer[1])

    def send_times(r, _):
        copy = pltpu.make_async_remote_copy(
            src_ref=dt_send, dst_ref=dt_recv.at[rank], send_sem=dt_ssem.at[r], recv_sem=dt_rsem.at[rank],
            device_id=place(r), device_id_type=MESH,
        )
        copy.start()
        return 0

    lax.fori_loop(rank + 1, n, send_times, 0)

    left = lax.broadcasted_iota(jnp.int32, (1, 128), 1) < size

    def unpack_rates(m):
        pack = rf_pack[m]
        flip = pltpu.roll(pack, size, 1)
        for kind in range(2):
            near, far = (pack, flip) if kind == 0 else (flip, pack)
            for b in range(blocks):
                row = jnp.where(left, near[2 * b:2 * b + 1], far[2 * b + 1:2 * b + 2])
                rf_all[m, kind:kind + 1, b * 128:(b + 1) * 128] = row
                rf8[m, kind, pl.ds(b, 1), :] = row
                rf8[m, kind, pl.ds(blocks + b, 1), :] = row

    unpack_rates(0)

    loads[1].wait()
    gain = gain_ref[...]

    def norm_strip(i, _):
        at = pl.ds(pl.multiple_of(i * STRIP, STRIP), STRIP)
        value = tok[at, :].astype(F32)
        scale = lax.rsqrt(jnp.mean(value * value, axis=1, keepdims=True) + 1e-6)
        normed[at, :] = (value * scale * gain).astype(BF16)
        return 0

    lax.fori_loop(0, rows // STRIP, norm_strip, 0)

    def forward(c, mine):
        base = own_half if mine else other_half
        part = pl.ds(pl.multiple_of(base + c * piece, 128), piece)
        way = 0 if mine else 2
        arrived(w_in.at[2, part], w_recv.at[way, c])
        if mine:
            send(w_in.at[2, part], w_in.at[2, part], w_send.at[2, c], w_recv.at[2, c], across)
        send(w_in.at[2, part], w_in.at[3, part], w_send.at[3 if mine else 4, c], w_recv.at[3 if mine else 4, c], peer[1])

    def tables(m):
        rate = rf_all[m, 0:1, :]
        freq = rf_all[m, 1:2, :]
        first = lax.broadcasted_iota(jnp.int32, (STRIP, lanes), 0) == 0

        def strip(i, before):
            br, bi = before
            at = pl.ds(pl.multiple_of(i * STRIP, STRIP), STRIP)
            t = times[at, 0:1]
            c, s = turn(t * freq)
            load = t * rate
            small = jnp.exp(-load)
            large = jnp.exp(load)
            pr, pi = small * c, small * s
            p_re[m, at, :] = pr
            p_im[m, at, :] = pi
            p_cat[m, at, 0:lanes] = pr.astype(BF16)
            p_cat[m, at, lanes:] = pi.astype(BF16)
            qr, qi = large * c, -large * s
            d_re[m, at, :] = jnp.where(first, pltpu.roll(br, 1, 0), pltpu.roll(qr, 1, 0)) - qr
            d_im[m, at, :] = jnp.where(first, pltpu.roll(bi, 1, 0), pltpu.roll(qi, 1, 0)) - qi
            return qr, qi

        lax.fori_loop(0, rows // STRIP, strip, (jnp.ones((STRIP, lanes), F32), jnp.zeros((STRIP, lanes), F32)))

    mask_r = lax.broadcasted_iota(jnp.int32, (128, 128), 0) // per
    mask_c = lax.broadcasted_iota(jnp.int32, (128, 128), 1) // size
    same = [mask_r == mask_c + 2 * b for b in range(blocks)]

    def spread(packed):
        value = packed.astype(F32)
        flip = pltpu.roll(value, size, 1)
        re, im = jnp.where(left, value, flip), jnp.where(left, flip, value)
        return [jnp.where(keep, re, 0.0) for keep in same], [jnp.where(keep, im, 0.0) for keep in same]

    def local(m):
        re, im = spread(bc_all[m, 0])
        tab[...] = jnp.concatenate(re + im, axis=1).astype(BF16)
        drive = jnp.dot(normed[...], w_in[m], **FORM).astype(BF16)
        acc[...] = jnp.dot(drive, tab[...], **FORM)

        def weigh(i, _):
            at = pl.ds(pl.multiple_of(i * STRIP, STRIP), STRIP)
            vr, vi = acc[at, 0:lanes], acc[at, lanes:]
            dr, di = d_re[m, at, :], d_im[m, at, :]
            wide[at, 0:lanes] = (dr * vr - di * vi).astype(BF16)
            wide[at, lanes:] = (dr * vi + di * vr).astype(BF16)
            return 0

        lax.fori_loop(0, rows // STRIP, weigh, 0)
        acc[...] = jnp.dot(lower, wide[...], **FORM)
        last = pl.ds(rows - 1, 1)
        for b in range(blocks):
            at = pl.ds(b * 128, 128)
            ar, ai = acc[last, at], acc[last, pl.ds(lanes + b * 128, 128)]
            pr, pi = p_re[m, last, at], p_im[m, last, at]
            e_send[m, pl.ds(b, 1), :] = pr * ar - pi * ai
            e_send[m, pl.ds(blocks + b, 1), :] = pr * ai + pi * ar
        owner = tp ^ m

        def send_end(r, _):
            copy = pltpu.make_async_remote_copy(
                src_ref=e_send.at[m], dst_ref=e_recv.at[rank, owner], send_sem=e_ssem.at[r, m],
                recv_sem=e_rsem.at[rank, owner], device_id=place(r), device_id_type=MESH,
            )
            copy.start()
            return 0

        lax.fori_loop(rank + 1, n, send_end, 0)

        def rotate(i, _):
            at = pl.ds(pl.multiple_of(i * STRIP, STRIP), STRIP)
            ar, ai = acc[at, 0:lanes], acc[at, lanes:]
            pr, pi = p_re[m, at, :], p_im[m, at, :]
            state[at, 0:lanes] = (pr * ar - pi * ai).astype(BF16)
            state[at, lanes:] = (pr * ai + pi * ar).astype(BF16)
            return 0

        lax.fori_loop(0, rows // STRIP, rotate, 0)
        re, im = spread(bc_all[m, 1])
        tab[...] = jnp.concatenate(re + [-value for value in im], axis=1).astype(BF16)
        y_loc[m] = lax.dot_general(state[...], tab[...], (((1,), (1,)), ((), ())), **FORM)

    tables(0)
    local(0)
    for m in range(1, n_tp):
        arrived(rf_pack.at[m], small_sem.at[m])
        unpack_rates(m)
    tables(1)
    for c in range(CHUNKS):
        forward(c, True)
    arrived(bc_all.at[2, grp], bc_recv.at[0])
    send(bc_all.at[2, grp], bc_all.at[2, grp], bc_send.at[2], bc_recv.at[2], across)
    send(bc_all.at[2, grp], bc_all.at[3, grp], bc_send.at[3], bc_recv.at[3], peer[1])
    tables(2)
    for c in range(CHUNKS):
        forward(c, False)
    arrived(bc_all.at[2, 1 - grp], bc_recv.at[2])
    send(bc_all.at[2, 1 - grp], bc_all.at[3, 1 - grp], bc_send.at[4], bc_recv.at[4], peer[1])
    arrived(w_in.at[1], w_recv.at[1, 0])
    arrived(bc_all.at[1], bc_recv.at[1])
    local(1)
    tables(3)
    local(2)
    sign = jnp.where(lax.broadcasted_iota(jnp.int32, (2 * blocks, 128), 0) < blocks, -1.0, 1.0)
    def weight(k, since):
        j = rank - 1 - k
        arrived(dt_recv.at[j], dt_rsem.at[j])
        for m in range(n_tp):
            c, s = turn(since * rf8[m, 1])
            shrink = jnp.exp(-since * rf8[m, 0])
            c_w[j, m] = shrink * c
            s_w[j, m] = shrink * s * sign
        return since + dt_recv[j]

    lax.fori_loop(0, rank, weight, jnp.zeros((1, 128), F32))

    for c in range(CHUNKS):
        arrived(w_in.at[3, pl.ds(pl.multiple_of(own_half + c * piece, 128), piece)], w_recv.at[3, c])
        arrived(w_in.at[3, pl.ds(pl.multiple_of(other_half + c * piece, 128), piece)], w_recv.at[4, c])
    arrived(bc_all.at[3, grp], bc_recv.at[3])
    arrived(bc_all.at[3, 1 - grp], bc_recv.at[4])
    local(3)

    total = jnp.zeros((rows, 1), F32)
    for m in range(n_tp):
        owner = tp ^ m

        def take(j, x):
            arrived(e_recv.at[j, owner], e_rsem.at[j, owner])
            value = e_recv[j, owner]
            return x + c_w[j, m] * value + s_w[j, m] * pltpu.roll(value, blocks, 0)

        x_ref[...] = lax.fori_loop(0, rank, take, jnp.zeros((2 * blocks, 128), F32))
        cr, ci = spread(bc_all[m, 1])
        for b in range(blocks):
            xr, xi = x_ref[pl.ds(b, 1), :], x_ref[pl.ds(blocks + b, 1), :]
            tab[:, b * 128:(b + 1) * 128] = (cr[b] * xr - ci[b] * xi).astype(BF16)
            tab[:, lanes + b * 128:lanes + (b + 1) * 128] = (-(cr[b] * xi + ci[b] * xr)).astype(BF16)
        v = y_loc[m] + lax.dot_general(p_cat[m], tab[...], (((1,), (1,)), ((), ())), **FORM)
        v = 0.5 * v * (1.0 + jnp.tanh(0.7978845608 * (v + 0.044715 * (v * v * v))))
        v = v.astype(BF16).astype(F32)
        y_loc[m] = v
        total = total + jnp.sum(v * v, axis=1, keepdims=True)
    scale = lax.rsqrt(total * (1.0 / (n_tp * 128)) + 1e-6)
    for m in range(n_tp):
        owner = tp ^ m
        out_ref[:, pl.ds(pl.multiple_of(owner * 128, 128), 128)] = (y_loc[m] * scale * ogain_ref[owner]).astype(BF16)
    for copy in started:
        copy.wait_send()

    def drain(r, _):
        pltpu.make_async_copy(dt_send, dt_send, dt_ssem.at[r]).wait()
        for m in range(n_tp):
            pltpu.make_async_copy(e_send.at[m], e_send.at[m], e_ssem.at[r, m]).wait()
        return 0

    lax.fori_loop(rank + 1, n, drain, 0)


def on_device(
    tokens, step, in_gain, in_proj, decay_rate, frequency, input_map, readout, out_gain, out_proj
):
    n_tp, n_sp = lax.axis_size("tp"), lax.axis_size("sp")
    n = n_tp * n_sp
    rows, width = tokens.shape
    groups, size = decay_rate.shape
    lanes = groups * size
    inner = input_map.shape[3]
    chans = groups * inner
    assert n_tp == 4 and chans == 128 and size == 64 and groups == 8 and lax.axis_size("grp") == 2
    maps = input_map.transpose(0, 1, 3, 2).reshape(2, chans, size)
    reads = readout.reshape(2, chans, size)
    vmem, dma = pltpu.VMEM, pltpu.SemaphoreType.DMA
    full = pl.BlockSpec(memory_space=pltpu.VMEM)
    away = pl.BlockSpec(memory_space=pl.ANY)
    tile = (2 * lanes // 128, 128)
    shaped = pl.pallas_call(
        functools.partial(kernel, n, n_tp),
        out_shape=jax.ShapeDtypeStruct((rows, n_tp * chans), BF16),
        in_specs=[away, full, full, away, full, full, full, full, full],
        out_specs=full,
        scratch_shapes=[
            vmem((rows, width), BF16), vmem((rows, width), BF16), vmem((n_tp, width, chans), BF16),
            vmem((n_tp, rows, lanes), F32), vmem((n_tp, rows, lanes), F32),
            vmem((n_tp, rows, lanes), F32), vmem((n_tp, rows, lanes), F32),
            vmem((n_tp, rows, 2 * lanes), BF16),
            vmem((n_tp, rows, chans), F32),
            vmem((rows, 2 * lanes), BF16), vmem((rows, 2 * lanes), F32), vmem((rows, 2 * lanes), BF16),
            vmem((rows, 128), F32), vmem((n_tp, groups, 2 * size), F32), vmem((n_tp, 2, lanes), F32),
            vmem((n_tp, 2, chans, 2 * size), BF16),
            vmem((n_tp, 2) + tile, F32),
            vmem((n_tp,) + tile, F32), vmem((n, n_tp) + tile, F32),
            vmem((1, 128), F32), vmem((n, 1, 128), F32),
            vmem((n, n_tp) + tile, F32), vmem((n, n_tp) + tile, F32), vmem(tile, F32),
            vmem((chans, 2 * lanes), BF16),
            dma((2,)), dma((n_tp,)), dma((n_tp,)), dma((5, CHUNKS)), dma((5, CHUNKS)), dma((5,)), dma((5,)),
            dma((n, n_tp)), dma((n, n_tp)), dma((n,)), dma((n,)),
        ],
        compiler_params=pltpu.CompilerParams(collective_id=0, has_side_effects=True, vmem_limit_bytes=60 * 2**20),
    )(
        tokens, step.reshape(1, -1), in_gain.reshape(1, width), in_proj, decay_rate, frequency, maps, reads,
        out_gain.reshape(n_tp, 1, chans),
    )
    return jnp.dot(shaped, out_proj, preferred_element_type=F32).astype(BF16)


def solution(mesh):
    placed = (
        P(("grp", "sp", "tp"), None),
        P(("grp", "sp")),
        P(),
        P(None, "tp"),
        P("tp", None),
        P("tp", None),
        P(None, "tp", None, None),
        P(None, "tp", None, None),
        P(),
        P(),
    )
    return jax.shard_map(
        on_device,
        mesh=mesh,
        in_specs=placed,
        out_specs=P(("grp", "sp", "tp"), None),
        check_vma=False,
    )
```

```python
import functools
import math

import jax
import jax.numpy as jnp
from jax import lax
from jax.experimental import pallas as pl
from jax.experimental.pallas import tpu as pltpu
from jax.sharding import PartitionSpec as P

F32 = jnp.float32
BF16 = jnp.bfloat16
MESH = pl.DeviceIdType.MESH
CHUNKS = 4
STRIP = 16
UNROLL = 4
COS = (0.9999992107823232, -19.738980355764078, 64.9286574210355, -85.2716215343227, 58.79049212023138, -21.071105627794083)
SIN = (6.28318491649543, -41.34158923268886, 81.59994332979169, -76.61447253134615, 41.34288235500672, -12.471243535733244)
WHOLE = 12582912.0
FORM = dict(preferred_element_type=F32)


def poly(coefs, z):
    total = coefs[-1] * z + coefs[-2]
    for value in coefs[-3::-1]:
        total = total * z + value
    return total


def turn(phase):
    r = phase - ((phase + WHOLE) - WHOLE)
    z = r * r
    return poly(COS, z), poly(SIN, z) * r


def kernel(
    n, n_tp, tok_hbm, step_ref, gain_ref, proj_hbm, rate_ref, freq_ref, map_ref, read_ref, ogain_ref, out_ref,
    tok, normed, w_in, p_re, p_im, d_re, d_im, p_cat, y_loc,
    wide, acc, state, times, rf_pack, rf_all, bc_all, rf8, e_send, e_recv, dt_send, dt_recv,
    c_w, s_w, x_ref, tab, drive, c_tab,
    load_sem, small_sem, small_send, w_recv, w_send, bc_recv, bc_send,
    e_rsem, e_ssem, dt_rsem, dt_ssem,
):
    grp, sp, tp = lax.axis_index("grp"), lax.axis_index("sp"), lax.axis_index("tp")
    rank = sp * n_tp + tp
    rows = tok.shape[0]
    depth = w_in.shape[1]
    half = depth // 2
    piece = half // CHUNKS
    lanes = rf_all.shape[-1]
    blocks = lanes // 128

    def place(r):
        return {"sp": r // n_tp, "tp": lax.rem(r, n_tp)}

    peer = [None] + [{"tp": tp ^ m} for m in range(1, n_tp)]
    across = {"grp": 1 - grp}

    loads = [
        pltpu.make_async_copy(proj_hbm, w_in.at[0], load_sem.at[0]),
        pltpu.make_async_copy(tok_hbm, tok, load_sem.at[1]),
    ]
    for copy in loads:
        copy.start()

    barrier = pltpu.get_barrier_semaphore()

    def greet(k, _):
        pl.semaphore_signal(barrier, inc=1, device_id=place(lax.rem(rank + k, n)), device_id_type=MESH)
        return 0

    lax.fori_loop(1, n, greet, 0)
    pl.semaphore_signal(barrier, inc=1, device_id=across, device_id_type=MESH)

    step_row = step_ref[:, pl.ds(pl.multiple_of(tp * rows, 128), rows)]
    row_id = lax.broadcasted_iota(jnp.int32, (rows, rows), 0)
    col_id = lax.broadcasted_iota(jnp.int32, (rows, rows), 1)
    causal = col_id <= row_id
    elapsed = jnp.sum(jnp.where(causal, jnp.broadcast_to(step_row, (rows, rows)), 0.0), axis=1, keepdims=True)
    times[...] = jnp.broadcast_to(elapsed, (rows, 128))
    dt_send[...] = jnp.broadcast_to(jnp.sum(step_row, axis=1, keepdims=True), (1, 128))
    lower = causal.astype(F32).astype(BF16)

    size = rate_ref.shape[1]
    per = map_ref.shape[1] // rate_ref.shape[0]
    rate, freq = rate_ref[...], freq_ref[...]
    rf_pack[0] = jnp.concatenate([rate, freq * (0.5 / math.pi)], axis=1)

    def rows_of(value):
        return jnp.concatenate([jnp.broadcast_to(value[g:g + 1], (per, size)) for g in range(value.shape[0])], axis=0)

    norm = 1.0 / (rate * rate + freq * freq)
    r_n, f_n = rows_of(-rate * norm), rows_of(freq * norm)
    bc_all[0, 0] = jnp.concatenate(
        [f_n * map_ref[1] + r_n * map_ref[0], r_n * map_ref[1] - f_n * map_ref[0]], axis=1
    ).astype(BF16)
    bc_all[0, 1] = jnp.concatenate([read_ref[0], read_ref[1]], axis=1).astype(BF16)

    left = lax.broadcasted_iota(jnp.int32, (1, 128), 1) < size

    def unpack_rates(m):
        pack = rf_pack[m]
        flip = pltpu.roll(pack, size, 1)
        for kind in range(2):
            near, far = (pack, flip) if kind == 0 else (flip, pack)
            for b in range(blocks):
                row = jnp.where(left, near[2 * b:2 * b + 1], far[2 * b + 1:2 * b + 2])
                rf_all[m, kind:kind + 1, b * 128:(b + 1) * 128] = row
                rf8[m, kind, pl.ds(b, 1), :] = row
                rf8[m, kind, pl.ds(blocks + b, 1), :] = row

    unpack_rates(0)

    loads[1].wait()
    gain = gain_ref[...]

    def norm_strip(i, _):
        at = pl.ds(pl.multiple_of(i * STRIP, STRIP), STRIP)
        value = tok[at, :].astype(F32)
        scale = lax.rsqrt(jnp.mean(value * value, axis=1, keepdims=True) + 1e-6)
        normed[at, :] = (value * scale * gain).astype(BF16)
        return 0

    lax.fori_loop(0, rows // STRIP, norm_strip, 0, unroll=2)

    def tables(m):
        rate = rf_all[m, 0:1, :]
        freq = rf_all[m, 1:2, :]
        first = lax.broadcasted_iota(jnp.int32, (STRIP, lanes), 0) == 0

        def strip(i, before):
            br, bi = before
            at = pl.ds(pl.multiple_of(i * STRIP, STRIP), STRIP)
            t = times[at, 0:1]
            c, s = turn(t * freq)
            load = t * rate
            small = jnp.exp(-load)
            large = jnp.exp(load)
            pr, pi = small * c, small * s
            p_re[m, at, :] = pr
            p_im[m, at, :] = pi
            p_cat[m, at, 0:lanes] = pr.astype(BF16)
            p_cat[m, at, lanes:] = pi.astype(BF16)
            qr, qi = large * c, -large * s
            d_re[m, at, :] = jnp.where(first, pltpu.roll(br, 1, 0), pltpu.roll(qr, 1, 0)) - qr
            d_im[m, at, :] = jnp.where(first, pltpu.roll(bi, 1, 0), pltpu.roll(qi, 1, 0)) - qi
            return qr, qi

        lax.fori_loop(0, rows // STRIP, strip, (jnp.ones((STRIP, lanes), F32), jnp.zeros((STRIP, lanes), F32)), unroll=UNROLL)

    tables(0)
    loads[0].wait()
    pl.semaphore_wait(barrier, n)

    started = []

    def send(src, dst, ssem, rsem, where):
        copy = pltpu.make_async_remote_copy(
            src_ref=src, dst_ref=dst, send_sem=ssem, recv_sem=rsem, device_id=where, device_id_type=MESH
        )
        copy.start()
        started.append(copy)
        return copy

    def arrived(dst, rsem):
        pltpu.make_async_copy(dst, dst, rsem).wait()

    for m in range(1, n_tp):
        send(rf_pack.at[0], rf_pack.at[m], small_send.at[m], small_sem.at[m], peer[m])
    own_half = grp * half
    other_half = (1 - grp) * half
    for c in range(CHUNKS):
        part = pl.ds(pl.multiple_of(own_half + c * piece, 128), piece)
        send(w_in.at[0, part], w_in.at[2, part], w_send.at[0, c], w_recv.at[0, c], peer[2])
    send(w_in.at[0], w_in.at[1], w_send.at[1, 0], w_recv.at[1, 0], peer[1])
    send(bc_all.at[0, grp], bc_all.at[2, grp], bc_send.at[0], bc_recv.at[0], peer[2])
    send(bc_all.at[0], bc_all.at[1], bc_send.at[1], bc_recv.at[1], peer[1])

    def send_times(r, _):
        copy = pltpu.make_async_remote_copy(
            src_ref=dt_send, dst_ref=dt_recv.at[rank], send_sem=dt_ssem.at[r], recv_sem=dt_rsem.at[rank],
            device_id=place(r), device_id_type=MESH,
        )
        copy.start()
        return 0

    lax.fori_loop(rank + 1, n, send_times, 0)

    def forward(c, mine):
        base = own_half if mine else other_half
        part = pl.ds(pl.multiple_of(base + c * piece, 128), piece)
        way = 0 if mine else 2
        arrived(w_in.at[2, part], w_recv.at[way, c])
        if mine:
            send(w_in.at[2, part], w_in.at[2, part], w_send.at[2, c], w_recv.at[2, c], across)
        send(w_in.at[2, part], w_in.at[3, part], w_send.at[3 if mine else 4, c], w_recv.at[3 if mine else 4, c], peer[1])

    mask_r = lax.broadcasted_iota(jnp.int32, (128, 128), 0) // per
    mask_c = lax.broadcasted_iota(jnp.int32, (128, 128), 1) // size
    same = [mask_r == mask_c + 2 * b for b in range(blocks)]

    def spread(packed):
        value = packed.astype(F32)
        flip = pltpu.roll(value, size, 1)
        re, im = jnp.where(left, value, flip), jnp.where(left, flip, value)
        return [jnp.where(keep, re, 0.0) for keep in same], [jnp.where(keep, im, 0.0) for keep in same]

    def project(m):
        pair = jnp.concatenate([w_in[m], w_in[m + 1]], axis=1)
        value = jnp.dot(normed[...], pair, **FORM).astype(BF16)
        drive[m] = value[:, 0:128]
        drive[m + 1] = value[:, 128:]

    def local(m):
        re, im = spread(bc_all[m, 0])
        tab[...] = jnp.concatenate(re + im, axis=1).astype(BF16)
        acc[...] = jnp.dot(drive[m], tab[...], **FORM)

        def weigh(i, _):
            at = pl.ds(pl.multiple_of(i * STRIP, STRIP), STRIP)
            vr, vi = acc[at, 0:lanes], acc[at, lanes:]
            dr, di = d_re[m, at, :], d_im[m, at, :]
            wide[at, 0:lanes] = (dr * vr - di * vi).astype(BF16)
            wide[at, lanes:] = (dr * vi + di * vr).astype(BF16)
            return 0

        lax.fori_loop(0, rows // STRIP, weigh, 0, unroll=4)
        acc[...] = jnp.dot(lower, wide[...], **FORM)
        last = pl.ds(rows - 1, 1)
        for b in range(blocks):
            at = pl.ds(b * 128, 128)
            ar, ai = acc[last, at], acc[last, pl.ds(lanes + b * 128, 128)]
            pr, pi = p_re[m, last, at], p_im[m, last, at]
            e_send[m, pl.ds(b, 1), :] = pr * ar - pi * ai
            e_send[m, pl.ds(blocks + b, 1), :] = pr * ai + pi * ar
        owner = tp ^ m

        def send_end(r, _):
            copy = pltpu.make_async_remote_copy(
                src_ref=e_send.at[m], dst_ref=e_recv.at[rank, owner], send_sem=e_ssem.at[r, m],
                recv_sem=e_rsem.at[rank, owner], device_id=place(r), device_id_type=MESH,
            )
            copy.start()
            return 0

        lax.fori_loop(rank + 1, n, send_end, 0)

        def rotate(i, _):
            at = pl.ds(pl.multiple_of(i * STRIP, STRIP), STRIP)
            ar, ai = acc[at, 0:lanes], acc[at, lanes:]
            pr, pi = p_re[m, at, :], p_im[m, at, :]
            state[at, 0:lanes] = (pr * ar - pi * ai).astype(BF16)
            state[at, lanes:] = (pr * ai + pi * ar).astype(BF16)
            return 0

        lax.fori_loop(0, rows // STRIP, rotate, 0, unroll=4)
        re, im = spread(bc_all[m, 1])
        for b in range(blocks):
            c_tab[m, :, b * 128:(b + 1) * 128] = re[b]
            c_tab[m, :, lanes + b * 128:lanes + (b + 1) * 128] = im[b]
        tab[...] = jnp.concatenate(re + [-value for value in im], axis=1).astype(BF16)
        y_loc[m] = lax.dot_general(state[...], tab[...], (((1,), (1,)), ((), ())), **FORM)

    for m in range(1, n_tp):
        arrived(rf_pack.at[m], small_sem.at[m])
        unpack_rates(m)
    tables(1)
    forward(0, True)
    tables(2)
    forward(1, True)
    arrived(w_in.at[1], w_recv.at[1, 0])
    arrived(bc_all.at[1], bc_recv.at[1])
    project(0)
    local(0)
    forward(2, True)
    forward(3, True)
    arrived(bc_all.at[2, grp], bc_recv.at[0])
    send(bc_all.at[2, grp], bc_all.at[2, grp], bc_send.at[2], bc_recv.at[2], across)
    send(bc_all.at[2, grp], bc_all.at[3, grp], bc_send.at[3], bc_recv.at[3], peer[1])
    local(1)
    forward(0, False)
    forward(1, False)
    forward(2, False)
    tables(3)
    forward(3, False)
    arrived(bc_all.at[2, 1 - grp], bc_recv.at[2])
    send(bc_all.at[2, 1 - grp], bc_all.at[3, 1 - grp], bc_send.at[4], bc_recv.at[4], peer[1])
    sign = jnp.where(lax.broadcasted_iota(jnp.int32, (2 * blocks, 128), 0) < blocks, -1.0, 1.0)
    def weight(k, since):
        j = rank - 1 - k
        arrived(dt_recv.at[j], dt_rsem.at[j])
        for m in range(n_tp):
            c, s = turn(since * rf8[m, 1])
            shrink = jnp.exp(-since * rf8[m, 0])
            c_w[j, m] = shrink * c
            s_w[j, m] = shrink * s * sign
        return since + dt_recv[j]

    lax.fori_loop(0, rank, weight, jnp.zeros((1, 128), F32))

    for c in range(CHUNKS):
        arrived(w_in.at[3, pl.ds(pl.multiple_of(own_half + c * piece, 128), piece)], w_recv.at[3, c])
        arrived(w_in.at[3, pl.ds(pl.multiple_of(other_half + c * piece, 128), piece)], w_recv.at[4, c])
    arrived(bc_all.at[3, grp], bc_recv.at[3])
    arrived(bc_all.at[3, 1 - grp], bc_recv.at[4])
    project(2)
    local(2)
    local(3)

    total = jnp.zeros((rows, 1), F32)
    for m in range(n_tp):
        owner = tp ^ m

        def take(j, x):
            arrived(e_recv.at[j, owner], e_rsem.at[j, owner])
            value = e_recv[j, owner]
            return x + c_w[j, m] * value + s_w[j, m] * pltpu.roll(value, blocks, 0)

        x_ref[...] = lax.fori_loop(0, rank, take, jnp.zeros((2 * blocks, 128), F32))
        for b in range(blocks):
            cr, ci = c_tab[m, :, b * 128:(b + 1) * 128], c_tab[m, :, lanes + b * 128:lanes + (b + 1) * 128]
            xr, xi = x_ref[pl.ds(b, 1), :], x_ref[pl.ds(blocks + b, 1), :]
            tab[:, b * 128:(b + 1) * 128] = (cr * xr - ci * xi).astype(BF16)
            tab[:, lanes + b * 128:lanes + (b + 1) * 128] = (-(cr * xi + ci * xr)).astype(BF16)
        v = y_loc[m] + lax.dot_general(p_cat[m], tab[...], (((1,), (1,)), ((), ())), **FORM)
        v = 0.5 * v * (1.0 + jnp.tanh(0.7978845608 * (v + 0.044715 * (v * v * v))))
        v = v.astype(BF16).astype(F32)
        y_loc[m] = v
        total = total + jnp.sum(v * v, axis=1, keepdims=True)
    scale = lax.rsqrt(total * (1.0 / (n_tp * 128)) + 1e-6)
    for m in range(n_tp):
        owner = tp ^ m
        out_ref[:, pl.ds(pl.multiple_of(owner * 128, 128), 128)] = (y_loc[m] * scale * ogain_ref[owner]).astype(BF16)
    for copy in started:
        copy.wait_send()

    def drain(r, _):
        pltpu.make_async_copy(dt_send, dt_send, dt_ssem.at[r]).wait()
        for m in range(n_tp):
            pltpu.make_async_copy(e_send.at[m], e_send.at[m], e_ssem.at[r, m]).wait()
        return 0

    lax.fori_loop(rank + 1, n, drain, 0)


def on_device(
    tokens, step, in_gain, in_proj, decay_rate, frequency, input_map, readout, out_gain, out_proj
):
    n_tp, n_sp = lax.axis_size("tp"), lax.axis_size("sp")
    n = n_tp * n_sp
    rows, width = tokens.shape
    groups, size = decay_rate.shape
    lanes = groups * size
    inner = input_map.shape[3]
    chans = groups * inner
    assert n_tp == 4 and chans == 128 and size == 64 and groups == 8 and lax.axis_size("grp") == 2
    maps = input_map.transpose(0, 1, 3, 2).reshape(2, chans, size)
    reads = readout.reshape(2, chans, size)
    vmem, dma = pltpu.VMEM, pltpu.SemaphoreType.DMA
    full = pl.BlockSpec(memory_space=pltpu.VMEM)
    away = pl.BlockSpec(memory_space=pl.ANY)
    tile = (2 * lanes // 128, 128)
    shaped = pl.pallas_call(
        functools.partial(kernel, n, n_tp),
        out_shape=jax.ShapeDtypeStruct((rows, n_tp * chans), BF16),
        in_specs=[away, full, full, away, full, full, full, full, full],
        out_specs=full,
        scratch_shapes=[
            vmem((rows, width), BF16), vmem((rows, width), BF16), vmem((n_tp, width, chans), BF16),
            vmem((n_tp, rows, lanes), F32), vmem((n_tp, rows, lanes), F32),
            vmem((n_tp, rows, lanes), F32), vmem((n_tp, rows, lanes), F32),
            vmem((n_tp, rows, 2 * lanes), BF16),
            vmem((n_tp, rows, chans), F32),
            vmem((rows, 2 * lanes), BF16), vmem((rows, 2 * lanes), F32), vmem((rows, 2 * lanes), BF16),
            vmem((rows, 128), F32), vmem((n_tp, groups, 2 * size), F32), vmem((n_tp, 2, lanes), F32),
            vmem((n_tp, 2, chans, 2 * size), BF16),
            vmem((n_tp, 2) + tile, F32),
            vmem((n_tp,) + tile, F32), vmem((n, n_tp) + tile, F32),
            vmem((1, 128), F32), vmem((n, 1, 128), F32),
            vmem((n, n_tp) + tile, F32), vmem((n, n_tp) + tile, F32), vmem(tile, F32),
            vmem((chans, 2 * lanes), BF16), vmem((n_tp, rows, chans), BF16), vmem((n_tp, chans, 2 * lanes), F32),
            dma((2,)), dma((n_tp,)), dma((n_tp,)), dma((5, CHUNKS)), dma((5, CHUNKS)), dma((5,)), dma((5,)),
            dma((n, n_tp)), dma((n, n_tp)), dma((n,)), dma((n,)),
        ],
        compiler_params=pltpu.CompilerParams(collective_id=0, has_side_effects=True, vmem_limit_bytes=60 * 2**20),
    )(
        tokens, step.reshape(1, -1), in_gain.reshape(1, width), in_proj, decay_rate, frequency, maps, reads,
        out_gain.reshape(n_tp, 1, chans),
    )
    return jnp.dot(shaped, out_proj, preferred_element_type=F32).astype(BF16)


def solution(mesh):
    placed = (
        P(("grp", "sp", "tp"), None),
        P(("grp", "sp")),
        P(),
        P(None, "tp"),
        P("tp", None),
        P("tp", None),
        P(None, "tp", None, None),
        P(None, "tp", None, None),
        P(),
        P(),
    )
    return jax.shard_map(
        on_device,
        mesh=mesh,
        in_specs=placed,
        out_specs=P(("grp", "sp", "tp"), None),
        check_vma=False,
    )
```
